32 devices in a mesh: ep: 4 (over y, x), tp: 8 (over z, core).
Axes of the slice: x: 2, y: 2, z: 4, core: 2. Of those that a mesh axis runs over, the one named last changes fastest.
Arguments:
- tokens: bfloat16 [128, 4096], P('ep'), may hold values from -6 to 6
- norm_gain: float32 [4096], replicated, may hold values from 0.1 to 1.9
- group_ids: int32 [128, 1], P('ep'), may hold values from 0 to 1; in each aligned block of 32 rows (0 to 31, 32 to 63, ...) at most 32 rows name the same one
- local_ids: int32 [128, 4], P('ep'), may hold values from 0 to 7, all different within a row
- group_gate: float32 [128], P('ep'), may hold values from 0.3 to 1
- expert_gate: float32 [128, 4], P('ep'), may hold values from 0.1 to 1
- lengths: int32 [32], P('ep'), may hold values from 1 to 4, 64 in all
- w_gate: bfloat16 [16, 1024, 4096], P('ep', 'tp'), may hold values from -0.09375 to 0.09375
- w_up: bfloat16 [16, 1024, 4096], P('ep', 'tp'), may hold values from -0.09375 to 0.09375
- w_down: bfloat16 [16, 1024, 4096], P('ep', None, 'tp'), may hold values from -0.1875 to 0.1875
Outputs:
- mixed: bfloat16 [128, 4096], P('ep', 'tp')
The draws below stay inside these ranges and needn't reach their ends.
Inputs may be any that keep to these rules, and one draw needn't show every extreme that they name: `group_ids`: among the 32 rows of one index of ep no group is named by more than 32 rows, and some index reaches 32. `local_ids`: each row names 4 different experts of its group. `lengths`: the first that many of a sequence's 4 positions are live.
All inputs are finite; a program needn't handle non-finite values. No bound on the sum of `lengths` on one device may be relied on, other than what follows from the above.
Results may differ from the reference program's by a relative error of at most 0.0065.
Values may be sent and summed in bfloat16 or wider, within the bound.
No kernel may reach another device: no remote copies, remote signals or barrier semaphores. Data moves between devices by JAX's collectives and lax.ppermute only.
A program may use at most 64 MiB of HBM per device.

```python
import math
import jax
import jax.numpy as jnp
import numpy as np
from jax import lax

D = 4096
FF = 1024
EXP_PER_GROUP = 8
TOP_K = 4
STEP_TOK = 4
TOK_DEV = 32
SEQS = 32
TOKENS = 128
EXPERTS = 16
GROUPS = 2
CAP = 32


def levels(own_key, dims, shards, smallest, largest):
    def one(position, parts):
        steps = jax.random.uniform(jax.random.fold_in(jax.random.fold_in(own_key, 6), position), (parts,), jnp.float32, smallest / len(shards), largest / len(shards))
        return jnp.repeat(jnp.exp(steps), dims[position] // parts).reshape((-1,) + (1,) * (len(dims) - position - 1))

    factor_of = one(*shards[0])
    for cut in shards[1:]:
        factor_of = factor_of * one(*cut)
    return factor_of


def choose_distinct(key, rows, number_of, top, lift):
    ranking = jax.random.permutation(jax.random.fold_in(key, 1), number_of)
    pull = ranking
    for power in range(3):
        pull = pull * pull // number_of
    pull = pull * lift // number_of
    tickets = jax.random.randint(jax.random.fold_in(key, 2), (rows, number_of), 0, 4096) + pull
    sure = jax.random.permutation(jax.random.fold_in(key, 3), rows)[jnp.arange(number_of) % rows]
    tickets = jnp.where(jnp.arange(rows)[:, None] == sure[None, :], 1 << 14, tickets)
    merit = tickets * number_of + jnp.arange(number_of)
    return lax.top_k(merit.astype(jnp.int32), top)[1].astype(jnp.int32)


def length_profile(amount, total, bound, lean):
    weights = [(1 << 20) // math.isqrt(standing ** lean) + 1 for standing in range(2, amount + 1)]
    surplus, holding = total - bound - (amount - 1), [1] * (amount - 1)
    while surplus > 0:
        free = [i for i in range(amount - 1) if holding[i] < bound]
        mass, budget = sum([weights[i] for i in free]), surplus
        for i in free:
            more = min(bound - holding[i], max(1, budget * weights[i] // mass), surplus)
            holding[i] = holding[i] + more
            surplus = surplus - more
    return np.array([bound] + holding)


def uneven(own_key, count, total, limit, slope):
    if count == 2:
        one = jax.random.randint(own_key, (), max(1, total - limit), min(limit, total - 1) + 1)
        return jnp.stack([one, total - one])
    tallies = jnp.asarray(length_profile(count, total, limit, slope), jnp.int32)
    couples = (count - 1) // 2
    giver, taker = tallies[1:1 + 2 * couples:2], tallies[2:2 + 2 * couples:2]
    slack = jnp.minimum(giver - 1, limit - taker)
    moved = jax.random.randint(jax.random.fold_in(own_key, 1), (couples,), 0, 1 << 20) % (slack + 1)
    tallies = tallies.at[1:1 + 2 * couples:2].set(giver - moved).at[2:2 + 2 * couples:2].set(taker + moved)
    return tallies[jax.random.permutation(jax.random.fold_in(own_key, 2), count)]


def shared_out(key, own, number, rows, count, top, bound, slope):
    ranking = jax.random.permutation(key, count)
    packed, usual = shares(count, rows * top, bound, slope, True), shares(count, rows * top, bound, slope, False)
    places = jnp.arange(count)

    def named(sizes, offset_by):
        used = int((sizes > 0).sum())
        fixed = max(1, used // 4)
        shifted = fixed + (places - fixed + offset_by * (used - fixed)) % max(1, count - fixed)
        return jnp.zeros((count,), jnp.int32).at[ranking[jnp.where(places < fixed, places, shifted)]].set(jnp.asarray(sizes, jnp.int32))

    sizes = jnp.where(number % 4 == 0, named(packed, number // 4), named(usual, number - number // 4 - 1))
    mixed = jax.random.permutation(jax.random.fold_in(own, 3), count)
    donor, sink = mixed[0:count // 2 * 2:2], mixed[1:count // 2 * 2:2]
    margin = jnp.minimum(sizes[donor] - 1, bound - sizes[sink]) // 2
    margin = jnp.where((donor == ranking[0]) | (sink == ranking[0]) | (sizes[sink] == 0), 0, jnp.maximum(margin, 0))
    shifted = jax.random.randint(jax.random.fold_in(own, 4), (count // 2,), 0, 1 << 20) % (margin + 1)
    sizes = sizes.at[donor].add(-shifted).at[sink].add(shifted)
    labels = jnp.searchsorted(jnp.cumsum(sizes), jnp.arange(rows * top), side="right").astype(jnp.int32)
    listing = labels.reshape(top, rows).T
    listing = listing[jax.random.permutation(jax.random.fold_in(own, 1), rows)]
    offset_by = jax.random.randint(jax.random.fold_in(own, 2), (rows, 1), 0, top)
    return jnp.take_along_axis(listing, (jnp.arange(top)[None, :] + offset_by) % top, axis=1)


def shares(number_of, total, reach, skew, full):
    portions = [(1 << 20) // math.isqrt(rank ** skew) + 1 for rank in range(1, number_of + 1)]
    largest = reach if full else min(reach, max(-(-total // number_of), total * portions[0] // sum(portions)))
    least = 1 if total - largest >= number_of - 1 else 0
    given, rest = [largest] + [least] * (number_of - 1), total - largest - least * (number_of - 1)
    while rest > 0:
        movable = [i for i in range(1, number_of) if given[i] < largest] or [i for i in range(1, number_of) if given[i] < reach]
        whole, budget = sum([portions[i] for i in movable]), rest
        for i in movable:
            extra = min(reach - given[i], max(1, budget * portions[i] // whole), rest)
            given[i] = given[i] + extra
            rest = rest - extra
    return np.array(given)


def noise(rng, dims, deviation, reach, cuts=(), held_as=jnp.bfloat16):
    array = jax.random.normal(rng, dims, jnp.float32) * deviation
    if len(cuts) > 0:
        array = levels(rng, dims, cuts, -0.22, 0.18) * array
    return jnp.clip(array, min=-reach, max=reach).astype(held_as)


def setup_inputs(seed: int = 0) -> dict:
    keys = jax.random.split(jax.random.key(seed), 11)
    tokens = noise(keys[0], (TOKENS, D), 1.0, 6.0, ((0, 4),))
    norm_gain = jnp.clip(1.0 + 0.18 * jax.random.normal(keys[1], (D,), jnp.float32), 0.1, 1.9)
    group_ids_keys = jax.random.split(jax.random.fold_in(keys[2], 1), TOKENS // TOK_DEV)
    group_ids_turns = jax.random.permutation(jax.random.fold_in(keys[2], 3), TOKENS // TOK_DEV)
    group_ids = jax.vmap(lambda own, number: shared_out(jax.random.fold_in(keys[2], 2), own, number, TOK_DEV, GROUPS, 1, CAP, 2))(group_ids_keys, group_ids_turns).reshape((TOKENS, 1))
    local_ids = choose_distinct(keys[3], TOKENS, EXP_PER_GROUP, TOP_K, 8192)
    group_gate = jnp.clip(jnp.exp(math.log(1.0) - 1.2039728 * jax.random.uniform(keys[4], (TOKENS,), jnp.float32) ** levels(keys[4], (TOKENS,), ((0, 4),), -0.2, 0.2)), 0.3, 1.0)
    expert_gate = jnp.clip(0.1 + 0.9 * jax.random.uniform(keys[5], (TOKENS, TOP_K), jnp.float32) ** levels(keys[5], (TOKENS, TOP_K), ((0, 4),), -0.2, 0.2), 0.1, 1.0)
    lengths = uneven(keys[6], SEQS, SEQS * STEP_TOK // 2, STEP_TOK, 2).astype(jnp.int32)
    w_gate = noise(keys[7], (EXPERTS, FF, D), D ** -0.5, 0.09375, ((0, 4), (1, 8)))
    w_up = noise(keys[8], (EXPERTS, FF, D), D ** -0.5, 0.09375, ((0, 4), (1, 8)))
    w_down = noise(keys[9], (EXPERTS, FF, D), FF ** -0.5, 0.1875, ((0, 4), (2, 8)))
    return {"tokens": tokens, "norm_gain": norm_gain, "group_ids": group_ids, "local_ids": local_ids, "group_gate": group_gate, "expert_gate": expert_gate, "lengths": lengths, "w_gate": w_gate, "w_up": w_up, "w_down": w_down}


def reference(tokens, norm_gain, group_ids, local_ids, group_gate, expert_gate, lengths, w_gate, w_up, w_down):
    values = tokens.astype(jnp.float32)
    scale = lax.rsqrt(lax.optimization_barrier(jnp.mean(values * values, axis=1, keepdims=True)) + 1e-06)
    normed = (values * scale * norm_gain).astype(jnp.bfloat16)
    places = jnp.arange(TOKENS, dtype=jnp.int32)
    live = (places % STEP_TOK < lengths[places // STEP_TOK]).astype(jnp.float32)
    chosen = group_ids * EXP_PER_GROUP + local_ids
    weights = expert_gate * (group_gate * live)[:, None]

    def add_expert(index, total):
        share = lax.optimization_barrier(jnp.sum(jnp.where(chosen == index, weights, jnp.zeros_like(weights)), axis=1))
        gate_part = jnp.dot(normed, w_gate[index].T, preferred_element_type=jnp.float32)
        up_part = jnp.dot(normed, w_up[index].T, preferred_element_type=jnp.float32)
        hidden = (jax.nn.silu(gate_part) * up_part).astype(jnp.bfloat16)
        result = jnp.dot(hidden, w_down[index], preferred_element_type=jnp.float32)
        return total + share[:, None] * result
    total = lax.fori_loop(0, EXPERTS, add_expert, jnp.zeros((TOKENS, D), jnp.float32))
    return total.astype(jnp.bfloat16)
```

```python
import functools

import jax
import jax.numpy as jnp
from jax import lax
from jax.experimental import pallas as pl
from jax.experimental.pallas import tpu as pltpu
from jax.sharding import PartitionSpec as P

EXP_PER_GROUP = 8
STEP_TOK = 4
LANES = 128


def norm_rows(tokens, norm_gain):
    values = tokens.astype(jnp.float32)
    scale = lax.rsqrt(jnp.mean(values * values, axis=1, keepdims=True) + 1e-06)
    return (values * scale * norm_gain).astype(jnp.bfloat16)


def live_mask(lengths, tok_rows):
    places = jnp.arange(tok_rows, dtype=jnp.int32)
    within = places % STEP_TOK
    owner = places // STEP_TOK
    seq_ids = jnp.arange(lengths.shape[0], dtype=jnp.int32)
    hits = (owner[:, None] == seq_ids[None, :]) & (within[:, None] < lengths[None, :])
    return jnp.any(hits, axis=1).astype(jnp.float32)


def expert_hidden(rows, w_gate, w_up):
    gate_part = jnp.einsum("rd,efd->ref", rows, w_gate, preferred_element_type=jnp.float32)
    up_part = jnp.einsum("rd,efd->ref", rows, w_up, preferred_element_type=jnp.float32)
    return (jax.nn.silu(gate_part) * up_part).astype(jnp.bfloat16)


def general(
    tokens, norm_gain, group_ids, local_ids, group_gate, expert_gate, lengths, w_gate, w_up, w_down
):
    highest = lax.Precision.HIGHEST
    tok_rows = tokens.shape[0]
    exp_dev = w_gate.shape[0]
    width_part = w_down.shape[2]
    ep_size = lax.axis_size("ep")
    groups = exp_dev * ep_size // EXP_PER_GROUP
    normed = norm_rows(tokens, norm_gain)
    live = live_mask(lengths, tok_rows)
    local_cols = jnp.arange(EXP_PER_GROUP, dtype=jnp.int32)
    picks = (local_ids[:, :, None] == local_cols[None, None, :]).astype(jnp.float32)
    weights = expert_gate * (group_gate * live)[:, None]
    dense = jnp.sum(picks * weights[:, :, None], axis=1)
    group_cols = jnp.arange(groups, dtype=jnp.int32)
    member_int = (group_ids == group_cols[None, :]).astype(jnp.int32)
    member = member_int.astype(jnp.float32)
    capacity = 2 * tok_rows // groups
    counts = jnp.cumsum(member_int, axis=0)
    rank = jnp.sum((counts - 1) * member_int, axis=1)
    slot_ids = jnp.arange(capacity, dtype=jnp.int32)
    select = member.T[:, None, :] * (rank[None, None, :] == slot_ids[None, :, None]).astype(
        jnp.float32
    )
    rows_by_group = jnp.einsum(
        "gct,td->gcd", select.astype(jnp.bfloat16), normed, preferred_element_type=jnp.float32
    ).astype(jnp.bfloat16)
    gates_by_group = jnp.einsum("gct,tl->gcl", select, dense, precision=highest)
    share = EXP_PER_GROUP // exp_dev
    send_rows = jnp.repeat(rows_by_group, share, axis=0)
    send_gates = gates_by_group.reshape(groups, capacity, share, exp_dev).transpose(0, 2, 1, 3)
    send_gates = send_gates.reshape(ep_size, capacity, exp_dev)
    recv_rows = lax.all_to_all(send_rows, "ep", split_axis=0, concat_axis=0, tiled=True)
    recv_gates = lax.all_to_all(send_gates, "ep", split_axis=0, concat_axis=0, tiled=True)
    slot_rows = recv_rows.reshape(ep_size * capacity, recv_rows.shape[2])
    slot_gates = recv_gates.reshape(ep_size * capacity, exp_dev)
    hidden = expert_hidden(slot_rows, w_gate, w_up)
    total = jnp.einsum(
        "ref,efd->red",
        lax.all_gather(hidden, "tp", axis=2, tiled=True),
        w_down,
        preferred_element_type=jnp.float32,
    )
    results = jnp.einsum("re,red->rd", slot_gates, total, precision=highest)
    results = results.reshape(ep_size, capacity, width_part)
    back = lax.all_to_all(results, "ep", split_axis=0, concat_axis=0, tiled=True)
    grouped = jnp.sum(back.reshape(groups, share, capacity, width_part), axis=1)
    mixed = jnp.einsum("gct,gcd->td", select, grouped, precision=highest)
    return mixed.astype(jnp.bfloat16)


def prep_kernel(tok, gain, gids, lids, ggate, egate, lens, own, send):
    rows, width = tok.shape
    half = width // 2
    top = lids.shape[1]
    values = tok[...].astype(jnp.float32)
    scale = lax.rsqrt(jnp.mean(values * values, axis=1, keepdims=True) + 1e-06)
    normed = (values * scale * gain[...]).astype(jnp.bfloat16)
    own[...] = normed
    core = lax.rem(lax.axis_index("tp"), 2)

    @pl.when(core == 0)
    def _():
        send[:, :half] = normed[:, :half]

    @pl.when(core == 1)
    def _():
        send[:, :half] = normed[:, half:]

    seqs = lens.shape[1]
    row_s = lax.broadcasted_iota(jnp.int32, (rows, seqs), 0)
    col_s = lax.broadcasted_iota(jnp.int32, (rows, seqs), 1)
    length = jnp.sum(jnp.where(row_s // STEP_TOK == col_s, lens[...], 0), axis=1, keepdims=True)
    place = lax.broadcasted_iota(jnp.int32, (rows, 1), 0) % STEP_TOK
    live = (place < length).astype(jnp.float32)
    row_r = lax.broadcasted_iota(jnp.int32, (rows, rows), 0)
    col_r = lax.broadcasted_iota(jnp.int32, (rows, rows), 1)
    group = jnp.sum(jnp.where(row_r == col_r, ggate[...], 0.0), axis=1, keepdims=True)
    weights = egate[...] * (group * live)
    coarse = weights.astype(jnp.bfloat16).astype(jnp.float32)
    fine = weights - coarse
    ids = (gids[...] * EXP_PER_GROUP + lids[...]).astype(jnp.float32)
    lane = lax.broadcasted_iota(jnp.int32, (rows, LANES), 1)
    meta = jnp.where(lane == 3 * top, live, 0.0)
    for j in range(top):
        meta = jnp.where(lane == j, ids[:, j : j + 1], meta)
        meta = jnp.where(lane == top + j, coarse[:, j : j + 1], meta)
        meta = jnp.where(lane == 2 * top + j, fine[:, j : j + 1], meta)
    send[:, half:] = meta.astype(jnp.bfloat16)


def hidden_kernel(top, ep_size, *refs):
    own, first = refs[0], refs[1]
    got = refs[2 : 1 + ep_size]
    other = refs[1 + ep_size : 2 * ep_size]
    w_gate, w_up, out, spread = refs[2 * ep_size : 2 * ep_size + 4]
    x, acc_g, acc_u = refs[2 * ep_size + 4 :]
    rows = own.shape[0]
    width = own.shape[1]
    half = width // 2
    exp_dev, ff_part, depth = w_gate.shape
    step = pl.program_id(0)

    @pl.when(step == 0)
    def _():
        x[:rows, :] = own[...]
        core = lax.rem(lax.axis_index("tp"), 2)
        mine = pl.multiple_of(core * half, LANES)
        partner = pl.multiple_of((1 - core) * half, LANES)
        for i in range(ep_size - 1):
            span = slice((i + 1) * rows, (i + 2) * rows)
            x[span, pl.ds(mine, half)] = got[i][:, :half]
            x[span, pl.ds(partner, half)] = other[i][:, :half]
        acc_g[...] = jnp.zeros_like(acc_g)
        acc_u[...] = jnp.zeros_like(acc_u)

    part = x[:, pl.ds(pl.multiple_of(step * depth, LANES), depth)]
    dims = (((1,), (1,)), ((), ()))
    wg = w_gate[...].reshape(exp_dev * ff_part, depth)
    wu = w_up[...].reshape(exp_dev * ff_part, depth)
    acc_g[...] += lax.dot_general(part, wg, dims, preferred_element_type=jnp.float32)
    acc_u[...] += lax.dot_general(part, wu, dims, preferred_element_type=jnp.float32)

    @pl.when(step == pl.num_programs(0) - 1)
    def _():
        meta = jnp.concatenate(
            [first[:, half:]] + [g[:, half:] for g in got], axis=0
        ).astype(jnp.float32)
        base = (lax.axis_index("ep") * exp_dev).astype(jnp.float32)
        total = meta.shape[0]
        live = meta[:, 3 * top : 3 * top + 1]
        here = jnp.zeros((total, 1), jnp.float32)
        for j in range(top):
            inside = (meta[:, j : j + 1] >= base) & (meta[:, j : j + 1] < base + exp_dev)
            here = here + inside.astype(jnp.float32)
        keep = jnp.where((here > 0.0) & (live > 0.0), 1.0, 0.0)
        r = lax.broadcasted_iota(jnp.int32, (total, total), 0)
        c = lax.broadcasted_iota(jnp.int32, (total, total), 1)
        below = jnp.where(c < r, 1.0, 0.0).astype(jnp.bfloat16)
        wide = jnp.broadcast_to(keep, (total, LANES)).astype(jnp.bfloat16)
        rank = jnp.dot(below, wide, preferred_element_type=jnp.float32)
        slots = out.shape[0]
        slot = lax.broadcasted_iota(jnp.int32, (total, LANES), 1).astype(jnp.float32)
        place = jnp.where((rank == slot) & (keep > 0.0), 1.0, 0.0)
        spread[...] = place[:, :slots].astype(jnp.bfloat16)
        gather = place.T[:slots, :].astype(jnp.bfloat16)
        parts = []
        for e in range(exp_dev):
            weight = jnp.zeros((total, 1), jnp.float32)
            for j in range(top):
                both = meta[:, top + j : top + j + 1] + meta[:, 2 * top + j : 2 * top + j + 1]
                weight = weight + jnp.where(meta[:, j : j + 1] == base + e, both, 0.0)
            g = acc_g[:, e * ff_part : (e + 1) * ff_part]
            u = acc_u[:, e * ff_part : (e + 1) * ff_part]
            h = g / (1.0 + jnp.exp(-g)) * u * weight
            parts.append(h.astype(jnp.bfloat16))
        hidden = jnp.concatenate(parts, axis=1)
        out[...] = jnp.dot(gather, hidden, preferred_element_type=jnp.float32).astype(jnp.bfloat16)


def down_kernel(pairs, ep_size, *refs):
    mine = refs[:pairs]
    other = refs[pairs : 2 * pairs]
    spread, w_down = refs[2 * pairs : 2 * pairs + 2]
    outs = refs[2 * pairs + 2 : 2 * pairs + 2 + ep_size]
    h, acc = refs[2 * pairs + 2 + ep_size :]
    exp_dev = pl.num_programs(0)
    ff = w_down.shape[1]
    step = pl.program_id(0)
    slots, flat = mine[0].shape
    experts = h.shape[0]
    ff_part = flat // experts
    tp_size = 2 * pairs

    @pl.when(step == 0)
    def _():
        me = lax.axis_index("tp")
        flip = me + 1 - 2 * lax.rem(me, 2)
        for start, pieces in ((me, mine), (flip, other)):
            for i in range(pairs):
                source = lax.rem(start - 2 * i + tp_size, tp_size)
                at = pl.multiple_of(source * ff_part, LANES)
                for e in range(experts):
                    h[e, :, pl.ds(at, ff_part)] = pieces[i][:, e * ff_part : (e + 1) * ff_part]
        acc[...] = jnp.zeros_like(acc)

    acc[...] += jnp.dot(h[step], w_down[0], preferred_element_type=jnp.float32)

    @pl.when(step == exp_dev - 1)
    def _():
        rows = outs[0].shape[0]
        packed = acc[...].astype(jnp.bfloat16)
        back = jnp.dot(spread[...], packed, preferred_element_type=jnp.float32)
        for i in range(ep_size):
            outs[i][...] = back[i * rows : (i + 1) * rows].astype(jnp.bfloat16)


def whole(shape):
    return pl.BlockSpec(shape, lambda *_: (0,) * len(shape))


def local(
    tokens, norm_gain, group_ids, local_ids, group_gate, expert_gate, lengths, w_gate, w_up, w_down
):
    exp_dev, ff_part, width = w_gate.shape
    rows = tokens.shape[0]
    top = local_ids.shape[1]
    ep_size = lax.axis_size("ep")
    tp_size = lax.axis_size("tp")
    width_part = w_down.shape[2]
    ff = w_down.shape[1]
    total = rows * ep_size
    slots = total // 2
    if ff_part % LANES or total > LANES or ep_size & (ep_size - 1) or exp_dev * ep_size > 256:
        return general(
            tokens,
            norm_gain,
            group_ids,
            local_ids,
            group_gate,
            expert_gate,
            lengths,
            w_gate,
            w_up,
            w_down,
        )
    bf = jnp.bfloat16
    half = width // 2
    own, send = pl.pallas_call(
        prep_kernel,
        out_shape=(
            jax.ShapeDtypeStruct((rows, width), bf),
            jax.ShapeDtypeStruct((rows, half + LANES), bf),
        ),
        name="prep",
    )(
        tokens,
        norm_gain.reshape(1, width),
        group_ids,
        local_ids,
        group_gate.reshape(1, rows),
        expert_gate,
        lengths.reshape(1, -1),
    )
    swap = [(i, i ^ 1) for i in range(tp_size)]
    got = [
        lax.ppermute(send, "ep", [(i, i ^ k) for i in range(ep_size)]) for k in range(1, ep_size)
    ]
    other = [lax.ppermute(g, "tp", swap) for g in got]
    depth = width // 4
    flat = exp_dev * ff_part
    wspec = pl.BlockSpec((exp_dev, ff_part, depth), lambda s: (0, 0, s))
    hidden, spread = pl.pallas_call(
        functools.partial(hidden_kernel, top, ep_size),
        grid=(width // depth,),
        in_specs=[whole(own.shape)] + [whole(send.shape)] * (2 * ep_size - 1) + [wspec, wspec],
        out_specs=(whole((slots, flat)), whole((total, slots))),
        out_shape=(
            jax.ShapeDtypeStruct((slots, flat), bf),
            jax.ShapeDtypeStruct((total, slots), bf),
        ),
        scratch_shapes=[
            pltpu.VMEM((total, width), bf),
            pltpu.VMEM((total, flat), jnp.float32),
            pltpu.VMEM((total, flat), jnp.float32),
        ],
        name="hidden",
    )(own, send, *got, *other, w_gate, w_up)
    pairs = tp_size // 2
    mine = [hidden] + [
        lax.ppermute(hidden, "tp", [(i, (i + 2 * k) % tp_size) for i in range(tp_size)])
        for k in range(1, pairs)
    ]
    far = [lax.ppermute(m, "tp", swap) for m in mine]
    outs = pl.pallas_call(
        functools.partial(down_kernel, pairs, ep_size),
        grid=(exp_dev,),
        in_specs=[whole((slots, flat))] * tp_size
        + [whole((total, slots)), pl.BlockSpec((1, ff, width_part), lambda s: (s, 0, 0))],
        out_specs=tuple(whole((rows, width_part)) for _ in range(ep_size)),
        out_shape=tuple(jax.ShapeDtypeStruct((rows, width_part), bf) for _ in range(ep_size)),
        scratch_shapes=[
            pltpu.VMEM((exp_dev, slots, ff), bf),
            pltpu.VMEM((slots, width_part), jnp.float32),
        ],
        name="down",
    )(*mine, *far, spread, w_down)
    mixed = outs[0].astype(jnp.float32)
    for k in range(1, ep_size):
        back = lax.ppermute(outs[k], "ep", [(i, i ^ k) for i in range(ep_size)])
        mixed = mixed + back.astype(jnp.float32)
    return mixed.astype(bf)


def solution(mesh):
    in_specs = (
        P("ep", None),
        P(),
        P("ep", None),
        P("ep", None),
        P("ep"),
        P("ep", None),
        P("ep"),
        P("ep", "tp", None),
        P("ep", "tp", None),
        P("ep", None, "tp"),
    )
    out_specs = P("ep", "tp")
    return jax.shard_map(local, mesh=mesh, in_specs=in_specs, out_specs=out_specs, check_vma=False)
```
